32 devices in a mesh: fs: 4 (over z), rep: 4 (over y, x), tp: 2 (over core).
Axes of the slice: x: 2, y: 2, z: 4, core: 2. Of those that a mesh axis runs over, the one named last changes fastest.
Arguments:
- saved_inputs: bfloat16 [12288, 2048], P(('fs', 'rep')), may hold values from -6 to 6
- query_cotangent: bfloat16 [12288, 1024], P(('fs', 'rep'), 'tp'), may hold values from -0.053955078 to 0.053955078
- value_cotangent: bfloat16 [12288, 2048], P(('fs', 'rep'), 'tp'), may hold values from -0.053955078 to 0.053955078
- query_weight: float32 [2048, 1024], P('fs', 'tp'), may hold values from -0.125 to 0.125
- value_weight: float32 [2048, 2048], P('fs', 'tp'), may hold values from -0.125 to 0.125
- query_factor: bfloat16 [2048, 256], P('fs'), as said below
- value_factor: bfloat16 [2048, 256], P('fs'), as said below
- query_first: float32 [256, 1024], P('rep', 'tp'), may hold values from -6 to 6
- query_second: float32 [256, 1024], P('rep', 'tp'), may hold values from 0.3 to 3
- value_first: float32 [256, 2048], P('rep', 'tp'), may hold values from -6 to 6
- value_second: float32 [256, 2048], P('rep', 'tp'), may hold values from 0.3 to 3
Outputs:
- query_direction: float32 [2048, 1024], P('fs', 'tp')
- value_direction: float32 [2048, 2048], P('fs', 'tp')
- query_master: float32 [2048, 1024], P('fs', 'tp')
- value_master: float32 [2048, 2048], P('fs', 'tp')
- query_first_new: float32 [256, 1024], P('rep', 'tp')
- query_second_new: float32 [256, 1024], P('rep', 'tp')
- value_first_new: float32 [256, 2048], P('rep', 'tp')
- value_second_new: float32 [256, 2048], P('rep', 'tp')
- query_copy: bfloat16 [2048, 1024], P(None, 'tp')
- value_copy: bfloat16 [2048, 2048], P(None, 'tp')
The draws below stay inside these ranges and needn't reach their ends.
Inputs may be any that keep to these rules, and one draw needn't show every extreme that they name: `query_factor`: A matrix of full rank. `value_factor`: A matrix of full rank.
All inputs are finite; a program needn't handle non-finite values.
Results may differ from the reference program's by a relative error of at most 0.012.
Values may be sent and summed in bfloat16 or wider, within the bound.
No kernel may reach another device: no remote copies, remote signals or barrier semaphores. Data moves between devices by JAX's collectives and lax.ppermute only.
A program may use at most 128 MiB of HBM per device.

```python
import math
import jax
import jax.numpy as jnp
from jax import lax

D = 2048
QK = 1024
VW = 2048
RANK = 256
TOKENS = 12288


def factor_draw(key):
    first_key, second_key = jax.random.split(key)
    positions = jnp.arange(D, dtype=jnp.float32)
    trend = jnp.exp(math.log(3.0) * positions / D)
    spread = jnp.exp(jax.random.uniform(first_key, (D, 1), jnp.float32, 0.0, math.log(10.0)))
    base = jax.random.normal(second_key, (D, RANK), jnp.float32)
    return (base * spread * trend[:, None] * (0.3 / math.sqrt(D))).astype(jnp.bfloat16)


def draw_query_factor(key, part):
    return factor_draw(jax.random.fold_in(key, 11))


def draw_value_factor(key, part):
    return factor_draw(jax.random.fold_in(key, 23))


def block_levels(stream_key, extent, pieces, least, top_value):
    def one(dim, parts):
        heights = jax.random.uniform(jax.random.fold_in(jax.random.fold_in(stream_key, 6), dim), (parts,), jnp.float32, least / len(pieces), top_value / len(pieces))
        return jnp.repeat(jnp.exp(heights), extent[dim] // parts).reshape((-1,) + (1,) * (len(extent) - dim - 1))

    factor_of = one(*pieces[0])
    for cut in pieces[1:]:
        factor_of = factor_of * one(*cut)
    return factor_of


def normal_values(key, extent, scale, bound, pieces=(), held_as=jnp.bfloat16):
    array = scale * jax.random.normal(key, extent, jnp.float32)
    if pieces:
        array = array * block_levels(key, extent, pieces, -0.22, 0.18)
    return jnp.clip(array, -bound, bound).astype(held_as)


def setup_inputs(seed: int = 0) -> dict:
    keys = jax.random.split(jax.random.key(seed), 12)
    return {
        "saved_inputs": normal_values(keys[0], (TOKENS, D), 1.0, 6.0, ((0, 16),)),
        "query_cotangent": normal_values(keys[1], (TOKENS, QK), (TOKENS ** -0.5), 0.053955078, ((0, 16), (1, 2))),
        "value_cotangent": normal_values(keys[2], (TOKENS, VW), (TOKENS ** -0.5), 0.053955078, ((0, 16), (1, 2))),
        "query_weight": normal_values(keys[3], (D, QK), D ** -0.5, 0.125, ((0, 4), (1, 2)), jnp.float32),
        "value_weight": normal_values(keys[4], (D, VW), D ** -0.5, 0.125, ((0, 4), (1, 2)), jnp.float32),
        "query_factor": draw_query_factor(jax.random.fold_in(keys[11], 71), 0),
        "value_factor": draw_value_factor(jax.random.fold_in(keys[11], 71), 0),
        "query_first": normal_values(keys[7], (RANK, QK), 1.0, 6.0, ((0, 4), (1, 2)), jnp.float32),
        "query_second": jnp.clip(jnp.exp(math.log(3.0) - 2.3025851 * jax.random.uniform(keys[8], (RANK, QK), jnp.float32) ** block_levels(keys[8], (RANK, QK), ((0, 4), (1, 2)), -0.2, 0.2)), 0.3, 3.0),
        "value_first": normal_values(keys[9], (RANK, VW), 1.0, 6.0, ((0, 4), (1, 2)), jnp.float32),
        "value_second": jnp.clip(jnp.exp(math.log(3.0) - 2.3025851 * jax.random.uniform(keys[10], (RANK, VW), jnp.float32) ** block_levels(keys[10], (RANK, VW), ((0, 4), (1, 2)), -0.2, 0.2)), 0.3, 3.0),
    }


BETA_ONE = 0.8
BETA_TWO = 0.9
EPS_RATIO = 1e-08
EPS_NORM = 1e-06
RATE = 0.02

def update_one(grad, factor, weight, first, second):
    wide = factor.astype(jnp.float32)
    projected = jnp.dot(wide.T, grad, precision=lax.Precision.HIGHEST)
    first_new = BETA_ONE * first + (1.0 - BETA_ONE) * projected
    second_new = BETA_TWO * second + (1.0 - BETA_TWO) * projected * projected
    ratio = first_new / (jnp.sqrt(second_new) + EPS_RATIO)
    raw_step = jnp.dot(wide, ratio, precision=lax.Precision.HIGHEST)
    direction = raw_step * lax.rsqrt(jnp.mean(raw_step * raw_step) + EPS_NORM)
    master = weight - RATE * direction
    return (direction, master, first_new, second_new, master.astype(jnp.bfloat16))

def reference(saved_inputs, query_cotangent, value_cotangent, query_weight, value_weight, query_factor, value_factor, query_first, query_second, value_first, value_second):
    dims = (((0,), (0,)), ((), ()))
    query_grad = lax.dot_general(saved_inputs, query_cotangent, dims, preferred_element_type=jnp.float32)
    value_grad = lax.dot_general(saved_inputs, value_cotangent, dims, preferred_element_type=jnp.float32)
    q_dir, q_master, q_first, q_second, q_copy = update_one(query_grad, query_factor, query_weight, query_first, query_second)
    v_dir, v_master, v_first, v_second, v_copy = update_one(value_grad, value_factor, value_weight, value_first, value_second)
    return (q_dir, v_dir, q_master, v_master, q_first, q_second, v_first, v_second, q_copy, v_copy)
```

```python
import functools

import jax
import jax.numpy as jnp
from jax import lax
from jax.experimental import pallas as pl
from jax.experimental.pallas import tpu as pltpu
from jax.sharding import PartitionSpec as P

BETA_ONE = 0.8
BETA_TWO = 0.9
EPS_RATIO = 1e-08
EPS_NORM = 1e-06
RATE = 0.02


BF = jnp.bfloat16
F32 = jnp.float32
VMEM = pl.BlockSpec(memory_space=pltpu.VMEM)
ANY = pl.BlockSpec(memory_space=pltpu.HBM)
TILE = 16


def swap(x, axis, n, k):
    return lax.ppermute(x, axis, [(i, i ^ k) for i in range(n)])


def rows_at(block, height):
    return pl.ds(pl.multiple_of(block * height, height), height)


def call(body, outs, n_in, scratch=(), limit=None, flops=0, nbytes=0, in_specs=None, out_specs=None, name=None):
    return pl.pallas_call(
        body,
        out_shape=outs,
        in_specs=in_specs or [VMEM] * n_in,
        out_specs=out_specs or [VMEM] * len(outs),
        scratch_shapes=list(scratch),
        compiler_params=pltpu.CompilerParams(vmem_limit_bytes=limit),
        cost_estimate=pl.CostEstimate(flops=flops, bytes_accessed=nbytes, transcendentals=0),
        name=name,
    )


def project_body(nf, nr, *refs):
    x, fq, fv, cq, cv = refs[:5]
    mine, other = refs[5 : 5 + nr], refs[5 + nr : 5 + 2 * nr]
    outs = refs[5 + 2 * nr : 5 + 3 * nr]
    fac, part = refs[5 + 3 * nr :]
    f, r, t = lax.axis_index("fs"), lax.axis_index("rep"), lax.axis_index("tp")
    dl = fq.shape[0]
    piece = dl // nr
    fac[0, rows_at(f, dl), :] = fq[...]
    fac[1, rows_at(f, dl), :] = fv[...]
    for k in range(1, nf):
        for j in range(nr):
            here = rows_at((f ^ k) * nr + (r ^ j), piece)
            fac[t, here, :] = mine[j][k - 1]
            fac[1 - t, here, :] = other[j][k - 1]
    nq = cq.shape[1]
    dims = (((0,), (0,)), ((), ()))
    yq = jnp.dot(x[...], fac[0], preferred_element_type=F32).astype(BF)
    part[:, :nq] = lax.dot_general(yq, cq[...], dims, preferred_element_type=F32).astype(BF)
    yv = jnp.dot(x[...], fac[1], preferred_element_type=F32).astype(BF)
    part[:, nq:] = lax.dot_general(yv, cv[...], dims, preferred_element_type=F32).astype(BF)
    h = part.shape[0] // nr
    for j in range(nr):
        outs[j][...] = part[rows_at(r ^ j, h), :]


def plane_sum_body(nf, nr, *refs):
    ins, own, rest, acc = refs[:nr], refs[nr], refs[nr + 1 : nr + nf], refs[nr + nf]
    f = lax.axis_index("fs")
    total = ins[0][...].astype(F32)
    for ref in ins[1:]:
        total += ref[...].astype(F32)
    acc[...] = total
    h = acc.shape[0] // nf
    own[...] = acc[rows_at(f, h), :]
    for k in range(1, nf):
        rest[k - 1][...] = acc[rows_at(f ^ k, h), :].astype(BF)


def line_sum_body(nf, *refs):
    total = refs[0][...]
    for ref in refs[1:nf]:
        total += ref[...].astype(F32)
    refs[nf][...] = total.astype(BF)


def moments_body(nf, nq, *refs):
    ins = refs[:nf]
    q1, q2, v1, v2 = refs[nf : nf + 4]
    q1n, q2n, v1n, v2n, ratio, proj = refs[nf + 4 :]
    f = lax.axis_index("fs")
    h = ins[0].shape[0]
    for k in range(nf):
        proj[rows_at(f ^ k, h), :] = ins[k][...].astype(F32)
    for cols, first, second, fo, so in (
        (slice(None, nq), q1, q2, q1n, q2n),
        (slice(nq, None), v1, v2, v1n, v2n),
    ):
        p = proj[:, cols]
        fn = BETA_ONE * first[...] + (1.0 - BETA_ONE) * p
        sn = BETA_TWO * second[...] + (1.0 - BETA_TWO) * p * p
        fo[...] = fn
        so[...] = sn
        ratio[:, cols] = (fn / (jnp.sqrt(sn) + EPS_RATIO)).astype(BF)


def gram_body(fac, out):
    dims = (((0,), (0,)), ((), ()))
    for s in range(2):
        out[s] = lax.dot_general(fac[s], fac[s], dims, preferred_element_type=F32)


def total_body(nr, nq, *refs):
    ins, gram, ratio, total = refs[:nr], refs[nr], refs[nr + 1], refs[nr + 2]
    r = lax.axis_index("rep")
    h = ins[0].shape[0]
    for j in range(nr):
        ratio[rows_at(r ^ j, h), :] = ins[j][...]
    for s, cols in ((0, slice(None, nq)), (1, slice(nq, None))):
        z = ratio[:, cols]
        g = gram[s]
        acc = None
        for _ in range(3):
            high = g.astype(BF)
            g = g - high.astype(F32)
            term = jnp.dot(high, z, preferred_element_type=F32)
            acc = term if acc is None else acc + term
        total[rows_at(s, 8), :] = jnp.broadcast_to(jnp.sum(acc * z.astype(F32), keepdims=True), (8, 128))


def final_body(nf, nr, nt, *refs):
    fac, ratio, tot, tot_in, wq_h, wv_h, z_h = refs[:7]
    p_h = refs[7 : 6 + nr]
    refs = refs[6 + nr :]
    qd_h, vd_h, qm_h, vm_h, qc_h, vc_h = refs[:6]
    raw, wq, wv, w, qd, vd, qm, vm, qc, vc, in_sem, out_sem = refs[6:]
    f, r = lax.axis_index("fs"), lax.axis_index("rep")
    dl, nq, nv = wq.shape[0], wq.shape[1], wv.shape[1]
    d = dl * nf
    piece = dl // nr
    loads = [
        pltpu.make_async_copy(wq_h, wq, in_sem.at[0]),
        pltpu.make_async_copy(wv_h, wv, in_sem.at[1]),
        pltpu.make_async_copy(z_h, w.at[0], in_sem.at[2]),
    ]
    for j in range(1, nr):
        loads.append(pltpu.make_async_copy(p_h[j - 1], w.at[j], in_sem.at[2 + j]))
    for c in loads:
        c.start()
    both = tot[...] + tot_in[...]
    sq = lax.rsqrt(both[0:1, 0:1] / (d * nq * nt) + EPS_NORM)
    sv = lax.rsqrt(both[8:9, 0:1] / (d * nv * nt) + EPS_NORM)
    stores = []
    for k in range(nf):
        raw[:, :nq] = jnp.dot(fac[0, rows_at(f ^ k, dl), :], ratio[:, :nq], preferred_element_type=F32) * sq
        raw[:, nq:] = jnp.dot(fac[1, rows_at(f ^ k, dl), :], ratio[:, nq:], preferred_element_type=F32) * sv
        if k == 0:
            loads[0].wait()
            loads[1].wait()
            qd[...] = raw[:, :nq]
            vd[...] = raw[:, nq:]
            qm[...] = wq[...] - RATE * raw[:, :nq]
            vm[...] = wv[...] - RATE * raw[:, nq:]
            qc[0] = (wq[...].astype(BF).astype(F32) - RATE * raw[:, :nq]).astype(BF)
            vc[0] = (wv[...].astype(BF).astype(F32) - RATE * raw[:, nq:]).astype(BF)
            stores += [
                pltpu.make_async_copy(qd, qd_h, out_sem.at[0]),
                pltpu.make_async_copy(vd, vd_h, out_sem.at[1]),
                pltpu.make_async_copy(qm, qm_h, out_sem.at[2]),
                pltpu.make_async_copy(vm, vm_h, out_sem.at[3]),
            ]
            for c in stores:
                c.start()
        else:
            if k == 1:
                for c in loads[2:]:
                    c.wait()
            for j in range(nr):
                here = rows_at(r ^ j, piece)
                wide = w[j, k - 1].astype(F32) - RATE * raw[here, :]
                qc[k, here, :] = wide[:, :nq].astype(BF)
                vc[k, here, :] = wide[:, nq:].astype(BF)
        new = [
            pltpu.make_async_copy(qc.at[k], qc_h.at[rows_at(f ^ k, dl), :], out_sem.at[4 + 2 * k]),
            pltpu.make_async_copy(vc.at[k], vc_h.at[rows_at(f ^ k, dl), :], out_sem.at[5 + 2 * k]),
        ]
        for c in new:
            c.start()
        stores += new
    for c in stores:
        c.wait()


def exchange(nf, nr, nt, xs, cq, cv, wq, wv, fq, fv, q1, q2, v1, v2):
    S = jax.ShapeDtypeStruct
    f, r, t = lax.axis_index("fs"), lax.axis_index("rep"), lax.axis_index("tp")
    dl, rank = fq.shape
    nq, nv = cq.shape[1], cv.shape[1]
    nc = nq + nv
    d = nf * dl
    piece = dl // nr
    tokens = xs.shape[0]

    def quarter(a):
        return lax.dynamic_slice_in_dim(a, r * piece, piece, 0)

    start = jnp.where(t == 0, quarter(fq), quarter(fv))
    zs = [swap(start, "fs", nf, k) for k in range(nf - 1, 0, -1)][::-1]
    stacked = jnp.stack(zs)
    mine = [stacked] + [swap(stacked, "rep", nr, j) for j in range(1, nr)]
    other = [swap(m, "tp", nt, 1) for m in mine]

    wide = jnp.concatenate([quarter(wq), quarter(wv)], axis=1).astype(BF)
    wz = jnp.stack([swap(wide, "fs", nf, k) for k in range(nf - 1, 0, -1)][::-1])
    wp = [swap(wz, "rep", nr, j) for j in range(1, nr)]

    h = rank // nr
    *parts, fac = call(
        functools.partial(project_body, nf, nr),
        [S((h, nc), BF)] * nr + [S((2, d, rank), BF)],
        5 + 2 * nr,
        [pltpu.VMEM((rank, nc), BF)],
        flops=2 * tokens * (d * 2 * rank + rank * nc),
        nbytes=2 * (tokens * (d + nc) + 4 * d * rank),
        name="project",
    )(xs, fq, fv, cq, cv, *mine, *other)
    (gram,) = call(gram_body, [S((2, rank, rank), F32)], 1, flops=4 * d * rank * rank, nbytes=4 * d * rank, name="gram")(fac)

    got = [parts[0]] + [swap(parts[j], "rep", nr, j) for j in range(1, nr)]
    g = h // nf
    own, *rest = call(
        functools.partial(plane_sum_body, nf, nr),
        [S((g, nc), F32)] + [S((g, nc), BF)] * (nf - 1),
        nr,
        [pltpu.VMEM((h, nc), F32)],
        name="plane_sum",
    )(*got)
    got = [own] + [swap(rest[k - 1], "fs", nf, k) for k in range(1, nf)]
    (proj,) = call(functools.partial(line_sum_body, nf), [S((g, nc), BF)], nf, name="line_sum")(*got)
    got = [proj] + [swap(proj, "fs", nf, k) for k in range(1, nf)]
    q1n, q2n, v1n, v2n, ratio = call(
        functools.partial(moments_body, nf, nq),
        [S((h, nq), F32)] * 2 + [S((h, nv), F32)] * 2 + [S((h, nc), BF)],
        nf + 4,
        [pltpu.VMEM((h, nc), F32)],
        name="moments",
    )(*got, q1, q2, v1, v2)
    got = [ratio] + [swap(ratio, "rep", nr, j) for j in range(1, nr)]
    ratios, total = call(
        functools.partial(total_body, nr, nq),
        [S((rank, nc), BF), S((16, 128), F32)],
        nr + 1,
        name="total",
    )(*got, gram)
    total_in = swap(total, "tp", nt, 1)
    qd, vd, qm, vm, qc, vc = call(
        functools.partial(final_body, nf, nr, nt),
        [S((dl, nq), F32), S((dl, nv), F32)] * 2 + [S((d, nq), BF), S((d, nv), BF)],
        7 + nr - 1,
        [
            pltpu.VMEM((dl, nc), F32),
            pltpu.VMEM((dl, nq), F32),
            pltpu.VMEM((dl, nv), F32),
            pltpu.VMEM((nr, nf - 1, piece, nc), BF),
            pltpu.VMEM((dl, nq), F32),
            pltpu.VMEM((dl, nv), F32),
            pltpu.VMEM((dl, nq), F32),
            pltpu.VMEM((dl, nv), F32),
            pltpu.VMEM((nf, dl, nq), BF),
            pltpu.VMEM((nf, dl, nv), BF),
            pltpu.SemaphoreType.DMA((2 + nr,)),
            pltpu.SemaphoreType.DMA((4 + 2 * nf,)),
        ],
        in_specs=[VMEM] * 4 + [ANY] * (2 + nr),
        out_specs=[ANY] * 6,
        flops=2 * d * rank * nc,
        nbytes=2 * d * nc * 2 + 12 * dl * nc,
        name="final",
    )(fac, ratios, total, total_in, wq, wv, wz, *wp)
    return qd, vd, qm, vm, q1n, q2n, v1n, v2n, qc, vc


def moments(projected, first, second):
    first_new = BETA_ONE * first + (1.0 - BETA_ONE) * projected
    second_new = BETA_TWO * second + (1.0 - BETA_TWO) * projected * projected
    ratio = first_new / (jnp.sqrt(second_new) + EPS_RATIO)
    return (first_new, second_new, ratio)


def collective(nf, nr, nt, xs, cq, cv, wq, wv, fq, fv, q1, q2, v1, v2):
    dims = (((0,), (0,)), ((), ()))
    highest = lax.Precision.HIGHEST

    def one(cot, weight, factor, first, second):
        grad = lax.dot_general(xs, cot, dims, preferred_element_type=F32)
        whole = lax.all_gather(factor, "fs", axis=0, tiled=True).astype(F32)
        proj = jnp.dot(whole.T, grad, precision=highest)
        proj = lax.psum_scatter(proj.astype(BF), "rep", scatter_dimension=0, tiled=True).astype(F32)
        first_new, second_new, ratio = moments(lax.psum(proj, "fs"), first, second)
        ratio = lax.all_gather(ratio, "rep", axis=0, tiled=True)
        raw = jnp.dot(factor.astype(F32), ratio, precision=highest)
        total = lax.psum(jnp.sum(raw * raw), ("fs", "tp"))
        size = raw.size * nf * nt
        direction = raw * lax.rsqrt(total / size + EPS_NORM)
        master = weight - RATE * direction
        copy = lax.all_gather(master.astype(BF), "fs", axis=0, tiled=True)
        return direction, master, first_new, second_new, copy

    qd, qm, q1n, q2n, qc = one(cq, wq, fq, q1, q2)
    vd, vm, v1n, v2n, vc = one(cv, wv, fv, v1, v2)
    return qd, vd, qm, vm, q1n, q2n, v1n, v2n, qc, vc


def local(nf, nr, nt, *args):
    rank = args[5].shape[1]
    fits = all(n & (n - 1) == 0 for n in (nf, nr)) and nt == 2 and rank % (nf * nr * TILE) == 0
    return (exchange if fits else collective)(nf, nr, nt, *args)


def solution(mesh):
    placed = (
        P(("fs", "rep"), None),
        P(("fs", "rep"), "tp"),
        P(("fs", "rep"), "tp"),
        P("fs", "tp"),
        P("fs", "tp"),
        P("fs", None),
        P("fs", None),
        P("rep", "tp"),
        P("rep", "tp"),
        P("rep", "tp"),
        P("rep", "tp"),
    )
    return jax.shard_map(
        functools.partial(local, mesh.shape["fs"], mesh.shape["rep"], mesh.shape["tp"]),
        mesh=mesh,
        in_specs=placed,
        out_specs=(P("fs", "tp"),) * 4 + (P("rep", "tp"),) * 4 + (P(None, "tp"),) * 2,
        check_vma=False,
    )
```

```python
import functools

import jax
import jax.numpy as jnp
from jax import lax
from jax.experimental import pallas as pl
from jax.experimental.pallas import tpu as pltpu
from jax.sharding import PartitionSpec as P


BETA_ONE = 0.8
BETA_TWO = 0.9
EPS_RATIO = 1e-08
EPS_NORM = 1e-06
RATE = 0.02


BF = jnp.bfloat16
F32 = jnp.float32
VMEM = pl.BlockSpec(memory_space=pltpu.VMEM)
ANY = pl.BlockSpec(memory_space=pltpu.HBM)
TILE = 16


def swap(x, axis, n, k):
    return lax.ppermute(x, axis, [(i, i ^ k) for i in range(n)])


def rows_at(block, height):
    return pl.ds(pl.multiple_of(block * height, height), height)


def call(body, outs, n_in, scratch=(), limit=8, flops=0, nbytes=0, in_specs=None, out_specs=None):
    return pl.pallas_call(
        body,
        out_shape=outs,
        in_specs=in_specs or [VMEM] * n_in,
        out_specs=out_specs or [VMEM] * len(outs),
        scratch_shapes=list(scratch),
        compiler_params=pltpu.CompilerParams(vmem_limit_bytes=limit << 20),
        cost_estimate=pl.CostEstimate(flops=flops, bytes_accessed=nbytes, transcendentals=0),
    )


def first_body(nr, fq, fv, out, sem):
    r, t = lax.axis_index("rep"), lax.axis_index("tp")
    here = rows_at(r, fq.shape[0] // nr)
    for n, ref in enumerate((fq, fv)):

        @pl.when(t == n)
        def _():
            move = pltpu.make_async_copy(ref.at[here, :], out, sem)
            move.start()
            move.wait()


def pack_body(nr, wq_h, wv_h, quarter, low, high, wq, wv, sem):
    r = lax.axis_index("rep")
    dl, nq = wq.shape
    loads = [pltpu.make_async_copy(wq_h, wq, sem.at[0]), pltpu.make_async_copy(wv_h, wv, sem.at[1])]
    for c in loads:
        c.start()
    for c in loads:
        c.wait()
    for out, here in ((quarter, rows_at(r, dl // nr)), (low, slice(0, dl // 2)), (high, slice(dl // 2, dl))):
        out[:, :nq] = wq[here, :].astype(BF)
        out[:, nq:] = wv[here, :].astype(BF)


def project_body(nf, nr, *refs):
    x, fq, fv, cq_h, cv_h = refs[:5]
    mine, other = refs[5 : 5 + nr], refs[5 + nr : 5 + 2 * nr]
    outs = refs[5 + 2 * nr : 5 + 3 * nr]
    fac, part, cq, cv, sem = refs[5 + 3 * nr :]
    loads = [pltpu.make_async_copy(cq_h, cq, sem.at[0]), pltpu.make_async_copy(cv_h, cv, sem.at[1])]
    for c in loads:
        c.start()
    f, r, t = lax.axis_index("fs"), lax.axis_index("rep"), lax.axis_index("tp")
    dl = fq.shape[0]
    piece = dl // nr
    fac[0, rows_at(f, dl), :] = fq[...]
    fac[1, rows_at(f, dl), :] = fv[...]
    for k in range(1, nf):
        for j in range(nr):
            here = rows_at((f ^ k) * nr + (r ^ j), piece)
            fac[t, here, :] = mine[j][k - 1]
            fac[1 - t, here, :] = other[j][k - 1]
    nq = cq.shape[1]
    dims = (((0,), (0,)), ((), ()))
    yq = jnp.dot(x[...], fac[0], preferred_element_type=F32).astype(BF)
    for c in loads:
        c.wait()
    part[:, :nq] = lax.dot_general(yq, cq[...], dims, preferred_element_type=F32).astype(BF)
    yv = jnp.dot(x[...], fac[1], preferred_element_type=F32).astype(BF)
    part[:, nq:] = lax.dot_general(yv, cv[...], dims, preferred_element_type=F32).astype(BF)
    h = part.shape[0] // nr
    for j in range(nr):
        outs[j][...] = part[rows_at(r ^ j, h), :]


def plane_sum_body(nf, nr, *refs):
    ins, own, rest, acc = refs[:nr], refs[nr], refs[nr + 1 : nr + nf], refs[nr + nf]
    f = lax.axis_index("fs")
    total = ins[0][...].astype(F32)
    for ref in ins[1:]:
        total += ref[...].astype(F32)
    acc[...] = total
    h = acc.shape[0] // nf
    own[...] = acc[rows_at(f, h), :]
    for k in range(1, nf):
        rest[k - 1][...] = acc[rows_at(f ^ k, h), :].astype(BF)


def line_sum_body(nf, *refs):
    total = refs[0][...]
    for ref in refs[1:nf]:
        total += ref[...].astype(F32)
    refs[nf][...] = total.astype(BF)


def moments_body(nf, nq, *refs):
    ins = refs[:nf]
    q1, q2, v1, v2 = refs[nf : nf + 4]
    q1n, q2n, v1n, v2n, ratio, proj = refs[nf + 4 :]
    f = lax.axis_index("fs")
    h = ins[0].shape[0]
    for k in range(nf):
        proj[rows_at(f ^ k, h), :] = ins[k][...].astype(F32)
    for cols, first, second, fo, so in (
        (slice(None, nq), q1, q2, q1n, q2n),
        (slice(nq, None), v1, v2, v1n, v2n),
    ):
        p = proj[:, cols]
        fn = BETA_ONE * first[...] + (1.0 - BETA_ONE) * p
        sn = BETA_TWO * second[...] + (1.0 - BETA_TWO) * p * p
        fo[...] = fn
        so[...] = sn
        ratio[:, cols] = (fn / (jnp.sqrt(sn) + EPS_RATIO)).astype(BF)


def gram_body(fac, out):
    dims = (((0,), (0,)), ((), ()))
    for s in range(2):
        out[s] = lax.dot_general(fac[s], fac[s], dims, preferred_element_type=F32)


def total_body(nr, nq, *refs):
    ins, gram, ratio, total = refs[:nr], refs[nr], refs[nr + 1], refs[nr + 2]
    r = lax.axis_index("rep")
    h = ins[0].shape[0]
    for j in range(nr):
        ratio[rows_at(r ^ j, h), :] = ins[j][...]
    for s, cols in ((0, slice(None, nq)), (1, slice(nq, None))):
        z = ratio[:, cols]
        g = gram[s]
        acc = None
        for _ in range(3):
            high = g.astype(BF)
            g = g - high.astype(F32)
            term = jnp.dot(high, z, preferred_element_type=F32)
            acc = term if acc is None else acc + term
        total[rows_at(s, 8), :] = jnp.broadcast_to(jnp.sum(acc * z.astype(F32), keepdims=True), (8, 128))


def final_body(nf, nr, nt, *refs):
    fac, ratio, tot, tot_in, wq, wv = refs[:6]
    near, far = refs[6:8], refs[8:-14]
    qd_h, vd_h, qm_h, vm_h, qc_h, vc_h, raw, qd, vd, qm, vm, qc, vc, sem = refs[-14:]
    f, r = lax.axis_index("fs"), lax.axis_index("rep")
    dl, nq, nv = wq.shape[0], wq.shape[1], wv.shape[1]
    half = (nq + nv) // 2
    d = dl * nf
    piece = dl // nr
    both = tot[...] + tot_in[...]
    sq = lax.rsqrt(both[0:1, 0:1] / (d * nq * nt) + EPS_NORM)
    sv = lax.rsqrt(both[8:9, 0:1] / (d * nv * nt) + EPS_NORM)
    stores = []

    def put(k, here, cols, w):
        value = (w.astype(F32) - RATE * raw[here, cols]).astype(BF)
        split = min(max(nq - cols.start, 0), cols.stop - cols.start)
        if split:
            qc[k, here, cols.start : cols.start + split] = value[:, :split]
        if split < cols.stop - cols.start:
            vc[k, here, cols.start + split - nq : cols.stop - nq] = value[:, split:]

    left, right, whole = slice(0, half), slice(half, 2 * half), slice(0, 2 * half)
    for k in range(nf):
        raw[:, :nq] = jnp.dot(fac[0, rows_at(f ^ k, dl), :], ratio[:, :nq], preferred_element_type=F32) * sq
        raw[:, nq:] = jnp.dot(fac[1, rows_at(f ^ k, dl), :], ratio[:, nq:], preferred_element_type=F32) * sv
        if k == 0:
            qd[...] = raw[:, :nq]
            vd[...] = raw[:, nq:]
            qm[...] = wq[...] - RATE * raw[:, :nq]
            vm[...] = wv[...] - RATE * raw[:, nq:]
            put(0, slice(None), slice(0, nq), wq[...].astype(BF))
            put(0, slice(None), slice(nq, nq + nv), wv[...].astype(BF))
            stores += [
                pltpu.make_async_copy(qd, qd_h, sem.at[0]),
                pltpu.make_async_copy(vd, vd_h, sem.at[1]),
                pltpu.make_async_copy(qm, qm_h, sem.at[2]),
                pltpu.make_async_copy(vm, vm_h, sem.at[3]),
            ]
            for c in stores:
                c.start()
        elif k == 1:
            put(1, slice(0, dl // 2), whole, near[0][...])
            put(1, slice(dl // 2, dl), whole, near[1][...])
        else:
            own_z, xa, yb, ya, xb = far[5 * (k - 2) : 5 * (k - 1)]
            put(k, rows_at(r, piece), whole, own_z[...])
            for cols, group in ((left, (xa[...], ya[0], ya[1])), (right, (xb[0], yb[...], xb[1]))):
                for m, w in enumerate(group):
                    put(k, rows_at(r ^ (m + 1), piece), cols, w)
        new = [
            pltpu.make_async_copy(qc.at[k], qc_h.at[rows_at(f ^ k, dl), :], sem.at[4 + 2 * k]),
            pltpu.make_async_copy(vc.at[k], vc_h.at[rows_at(f ^ k, dl), :], sem.at[5 + 2 * k]),
        ]
        for c in new:
            c.start()
        stores += new
    for c in stores:
        c.wait()


def exchange(nf, nr, nt, xs, cq, cv, wq, wv, fq, fv, q1, q2, v1, v2):
    S = jax.ShapeDtypeStruct
    dl, rank = fq.shape
    nq, nv = cq.shape[1], cv.shape[1]
    nc = nq + nv
    half = nc // 2
    d = nf * dl
    piece = dl // nr
    tokens = xs.shape[0]

    (start,) = call(functools.partial(first_body, nr), [S((piece, rank), BF)], 2, [pltpu.SemaphoreType.DMA], limit=60, in_specs=[ANY] * 2)(fq, fv)
    zs = [swap(start, "fs", nf, k) for k in range(1, nf)]
    stacked = jnp.stack(zs)
    mine = [stacked] + [swap(stacked, "rep", nr, j) for j in range(1, nr)]
    other = [swap(m, "tp", nt, 1) for m in mine]

    quarter, low, high = call(
        functools.partial(pack_body, nr),
        [S((piece, nc), BF)] + [S((dl // 2, nc), BF)] * 2,
        2,
        [pltpu.VMEM((dl, nq), F32), pltpu.VMEM((dl, nv), F32), pltpu.SemaphoreType.DMA((2,))],
        in_specs=[ANY] * 2,
        limit=12,
    )(wq, wv)
    near = [swap(low, "fs", nf, 1), swap(high, "fs", nf, 1)]
    far = []
    for k in range(2, nf):
        own_z = swap(quarter, "fs", nf, k)
        fa, fb = own_z[:, :half], own_z[:, half:]
        xa = swap(fa, "rep", nr, 1)
        yb = swap(fb, "rep", nr, 2)
        ya = swap(jnp.stack([fa, xa]), "rep", nr, 2)
        xb = swap(jnp.stack([fb, yb]), "rep", nr, 1)
        far += [own_z, xa, yb, ya, xb]

    h = rank // nr
    *parts, fac = call(
        functools.partial(project_body, nf, nr),
        [S((h, nc), BF)] * nr + [S((2, d, rank), BF)],
        5 + 2 * nr,
        [
            pltpu.VMEM((rank, nc), BF),
            pltpu.VMEM(cq.shape, BF),
            pltpu.VMEM(cv.shape, BF),
            pltpu.SemaphoreType.DMA((2,)),
        ],
        limit=24,
        in_specs=[VMEM] * 3 + [ANY] * 2 + [VMEM] * 2 * nr,
        flops=2 * tokens * (d * 2 * rank + rank * nc),
        nbytes=2 * (tokens * (d + nc) + 4 * d * rank),
    )(xs, fq, fv, cq, cv, *mine, *other)
    (gram,) = call(gram_body, [S((2, rank, rank), F32)], 1, flops=4 * d * rank * rank, nbytes=4 * d * rank)(fac)

    got = [parts[0]] + [swap(parts[j], "rep", nr, j) for j in range(1, nr)]
    g = h // nf
    own, *rest = call(
        functools.partial(plane_sum_body, nf, nr),
        [S((g, nc), F32)] + [S((g, nc), BF)] * (nf - 1),
        nr,
        [pltpu.VMEM((h, nc), F32)],
    )(*got)
    got = [own] + [swap(rest[k - 1], "fs", nf, k) for k in range(1, nf)]
    (proj,) = call(functools.partial(line_sum_body, nf), [S((g, nc), BF)], nf)(*got)
    got = [proj] + [swap(proj, "fs", nf, k) for k in range(1, nf)]
    q1n, q2n, v1n, v2n, ratio = call(
        functools.partial(moments_body, nf, nq),
        [S((h, nq), F32)] * 2 + [S((h, nv), F32)] * 2 + [S((h, nc), BF)],
        nf + 4,
        [pltpu.VMEM((h, nc), F32)],
    )(*got, q1, q2, v1, v2)
    got = [ratio] + [swap(ratio, "rep", nr, j) for j in range(1, nr)]
    ratios, total = call(
        functools.partial(total_body, nr, nq), [S((rank, nc), BF), S((16, 128), F32)], nr + 1, limit=12
    )(*got, gram)
    total_in = swap(total, "tp", nt, 1)
    return (
        *call(
            functools.partial(final_body, nf, nr, nt),
            [S((dl, nq), F32), S((dl, nv), F32)] * 2 + [S((d, nq), BF), S((d, nv), BF)],
            8 + 5 * (nf - 2),
            [
                pltpu.VMEM((dl, nc), F32),
                pltpu.VMEM((dl, nq), F32),
                pltpu.VMEM((dl, nv), F32),
                pltpu.VMEM((dl, nq), F32),
                pltpu.VMEM((dl, nv), F32),
                pltpu.VMEM((nf, dl, nq), BF),
                pltpu.VMEM((nf, dl, nv), BF),
                pltpu.SemaphoreType.DMA((4 + 2 * nf,)),
            ],
            limit=36,
            out_specs=[ANY] * 6,
            flops=2 * d * rank * nc,
            nbytes=2 * d * nc * 2 + 12 * dl * nc,
        )(fac, ratios, total, total_in, wq, wv, *near, *far),
        q1n, q2n, v1n, v2n,
    )


def moments(projected, first, second):
    first_new = BETA_ONE * first + (1.0 - BETA_ONE) * projected
    second_new = BETA_TWO * second + (1.0 - BETA_TWO) * projected * projected
    ratio = first_new / (jnp.sqrt(second_new) + EPS_RATIO)
    return (first_new, second_new, ratio)


def collective(nf, nt, xs, cq, cv, wq, wv, fq, fv, q1, q2, v1, v2):
    dims = (((0,), (0,)), ((), ()))
    highest = lax.Precision.HIGHEST

    def one(cot, weight, factor, first, second):
        grad = lax.dot_general(xs, cot, dims, preferred_element_type=F32)
        whole = lax.all_gather(factor, "fs", axis=0, tiled=True).astype(F32)
        proj = jnp.dot(whole.T, grad, precision=highest)
        proj = lax.psum_scatter(proj.astype(BF), "rep", scatter_dimension=0, tiled=True).astype(F32)
        first_new, second_new, ratio = moments(lax.psum(proj, "fs"), first, second)
        ratio = lax.all_gather(ratio, "rep", axis=0, tiled=True)
        raw = jnp.dot(factor.astype(F32), ratio, precision=highest)
        total = lax.psum(jnp.sum(raw * raw), ("fs", "tp"))
        size = raw.size * nf * nt
        direction = raw * lax.rsqrt(total / size + EPS_NORM)
        master = weight - RATE * direction
        copy = lax.all_gather(master.astype(BF), "fs", axis=0, tiled=True)
        return direction, master, first_new, second_new, copy

    qd, qm, q1n, q2n, qc = one(cq, wq, fq, q1, q2)
    vd, vm, v1n, v2n, vc = one(cv, wv, fv, v1, v2)
    return qd, vd, qm, vm, q1n, q2n, v1n, v2n, qc, vc


def local(nf, nr, nt, *args):
    rank = args[5].shape[1]
    if not square(nf, nr, nt) or rank % (nf * nr * TILE):
        return collective(nf, nt, *args)
    qd, vd, qm, vm, qc, vc, *new = exchange(nf, nr, nt, *args)
    return qd, vd, qm, vm, *new, qc, vc


def square(nf, nr, nt):
    return (nf, nr, nt) == (4, 2 * 2, 2)


def solution(mesh):
    placed = (
        P(("fs", "rep"), None),
        P(("fs", "rep"), "tp"),
        P(("fs", "rep"), "tp"),
        P("fs", "tp"),
        P("fs", "tp"),
        P("fs", None),
        P("fs", None),
        P("rep", "tp"),
        P("rep", "tp"),
        P("rep", "tp"),
        P("rep", "tp"),
    )
    return jax.shard_map(
        functools.partial(local, mesh.shape["fs"], mesh.shape["rep"], mesh.shape["tp"]),
        mesh=mesh,
        in_specs=placed,
        out_specs=(P("fs", "tp"),) * 4 + (P("rep", "tp"),) * 4 + (P(None, "tp"),) * 2,
        check_vma=False,
    )
```

```python
import functools

import jax
import jax.numpy as jnp
from jax import lax
from jax.experimental import pallas as pl
from jax.experimental.pallas import tpu as pltpu
from jax.sharding import PartitionSpec as P


BETA_ONE = 0.8
BETA_TWO = 0.9
EPS_RATIO = 1e-08
EPS_NORM = 1e-06
RATE = 0.02


BF = jnp.bfloat16
F32 = jnp.float32
VMEM = pl.BlockSpec(memory_space=pltpu.VMEM)
ANY = pl.BlockSpec(memory_space=pltpu.HBM)
TILE = 16

def swap(x, axis, n, k):
    return lax.ppermute(x, axis, [(i, i ^ k) for i in range(n)])

def rows_at(block, height):
    return pl.ds(pl.multiple_of(block * height, height), height)

def call(body, outs, n_in, scratch=(), limit=8, flops=0, nbytes=0, in_specs=None, out_specs=None, aliases=None):
    return pl.pallas_call(
        body,
        out_shape=outs,
        in_specs=in_specs or [VMEM] * n_in,
        out_specs=out_specs or [VMEM] * len(outs),
        scratch_shapes=list(scratch),
        input_output_aliases=aliases or {},
        compiler_params=pltpu.CompilerParams(vmem_limit_bytes=limit << 20),
        cost_estimate=pl.CostEstimate(flops=flops, bytes_accessed=nbytes, transcendentals=0),
    )

def first_body(nr, fq, fv, out, sem):
    r, t = lax.axis_index("rep"), lax.axis_index("tp")
    here = rows_at(r, fq.shape[0] // nr)
    for n, ref in enumerate((fq, fv)):

        @pl.when(t == n)
        def _():
            move = pltpu.make_async_copy(ref.at[here, :], out, sem)
            move.start()
            move.wait()

def pack_body(nr, wq_h, wv_h, quarter, low, high, wq, wv, sem):
    r = lax.axis_index("rep")
    dl, nq = wq.shape
    loads = [pltpu.make_async_copy(wq_h, wq, sem.at[0]), pltpu.make_async_copy(wv_h, wv, sem.at[1])]
    for c in loads:
        c.start()
    for c in loads:
        c.wait()
    for out, here in ((quarter, rows_at(r, dl // nr)), (low, slice(0, dl // 2)), (high, slice(dl // 2, dl))):
        out[:, :nq] = wq[here, :].astype(BF)
        out[:, nq:] = wv[here, :].astype(BF)

def project_body(nf, nr, nq, *refs):
    x, fq, fv, cot = refs[:4]
    mine, other = refs[4 : 4 + nr], refs[4 + nr : 4 + 2 * nr]
    outs = refs[4 + 2 * nr : 4 + 3 * nr]
    fac, part = refs[4 + 3 * nr :]
    f, r, t = lax.axis_index("fs"), lax.axis_index("rep"), lax.axis_index("tp")
    dl = fq.shape[0]
    piece = dl // nr
    fac[0, rows_at(f, dl), :] = fq[...]
    fac[1, rows_at(f, dl), :] = fv[...]
    for k in range(1, nf):
        for j in range(nr):
            here = rows_at((f ^ k) * nr + (r ^ j), piece)
            fac[t, here, :] = mine[j][k - 1]
            fac[1 - t, here, :] = other[j][k - 1]
    dims = (((0,), (0,)), ((), ()))
    yq = jnp.dot(x[...], fac[0], preferred_element_type=F32).astype(BF)
    part[:, :nq] = lax.dot_general(yq, cot[:, :nq], dims, preferred_element_type=F32).astype(BF)
    yv = jnp.dot(x[...], fac[1], preferred_element_type=F32).astype(BF)
    part[:, nq:] = lax.dot_general(yv, cot[:, nq:], dims, preferred_element_type=F32).astype(BF)
    h = part.shape[0] // nr
    for j in range(nr):
        outs[j][...] = part[rows_at(r ^ j, h), :]

def plane_sum_body(nf, nr, *refs):
    ins, own, rest, acc = refs[:nr], refs[nr], refs[nr + 1 : nr + nf], refs[nr + nf]
    f = lax.axis_index("fs")
    total = ins[0][...].astype(F32)
    for ref in ins[1:]:
        total += ref[...].astype(F32)
    acc[...] = total
    h = acc.shape[0] // nf
    own[...] = acc[rows_at(f, h), :]
    for k in range(1, nf):
        rest[k - 1][...] = acc[rows_at(f ^ k, h), :].astype(BF)

def line_sum_body(nf, *refs):
    total = refs[0][...]
    for ref in refs[1:nf]:
        total += ref[...].astype(F32)
    refs[nf][...] = total.astype(BF)

def moments_body(nf, nq, *refs):
    ins = refs[:nf]
    q1, q2, v1, v2 = refs[nf : nf + 4]
    q1n, q2n, v1n, v2n, ratio, proj = refs[nf + 4 :]
    f = lax.axis_index("fs")
    h = ins[0].shape[0]
    for k in range(nf):
        proj[rows_at(f ^ k, h), :] = ins[k][...].astype(F32)
    for cols, first, second, fo, so in (
        (slice(None, nq), q1, q2, q1n, q2n),
        (slice(nq, None), v1, v2, v1n, v2n),
    ):
        p = proj[:, cols]
        fn = BETA_ONE * first[...] + (1.0 - BETA_ONE) * p
        sn = BETA_TWO * second[...] + (1.0 - BETA_TWO) * p * p
        fo[...] = fn
        so[...] = sn
        ratio[:, cols] = (fn / (jnp.sqrt(sn) + EPS_RATIO)).astype(BF)

def gram_body(fac, out):
    dims = (((0,), (0,)), ((), ()))
    for s in range(2):
        out[s] = lax.dot_general(fac[s], fac[s], dims, preferred_element_type=F32)

def total_body(nr, nq, *refs):
    ins, gram, ratio, total = refs[:nr], refs[nr], refs[nr + 1], refs[nr + 2]
    r = lax.axis_index("rep")
    h = ins[0].shape[0]
    for j in range(nr):
        ratio[rows_at(r ^ j, h), :] = ins[j][...]
    for s, cols in ((0, slice(None, nq)), (1, slice(nq, None))):
        z = ratio[:, cols]
        g = gram[s]
        acc = None
        for _ in range(3):
            high = g.astype(BF)
            g = g - high.astype(F32)
            term = jnp.dot(high, z, preferred_element_type=F32)
            acc = term if acc is None else acc + term
        total[rows_at(s, 8), :] = jnp.broadcast_to(jnp.sum(acc * z.astype(F32), keepdims=True), (8, 128))

def scales(fac, tot, tot_in, nq, nv, nt):
    both = tot[...] + tot_in[...]
    d = fac.shape[1]
    return (
        lax.rsqrt(both[0:1, 0:1] / (d * nq * nt) + EPS_NORM),
        lax.rsqrt(both[8:9, 0:1] / (d * nv * nt) + EPS_NORM),
    )

def step_rows(fac, ratio, raw, here, nq, scale):
    for s, cols in ((0, slice(None, nq)), (1, slice(nq, None))):
        raw[:, cols] = jnp.dot(fac[s, here, :], ratio[:, cols], preferred_element_type=F32) * scale[s]

def put(raw, qc, vc, slot, here, cols, w):
    nq = qc.shape[2]
    value = (w.astype(F32) - RATE * raw[here, cols]).astype(BF)
    split = min(max(nq - cols.start, 0), cols.stop - cols.start)
    if split:
        qc[slot, here, cols.start : cols.start + split] = value[:, :split]
    if split < cols.stop - cols.start:
        vc[slot, here, cols.start + split - nq : cols.stop - nq] = value[:, split:]

def put_far(raw, qc, vc, slot, pieces):
    own_z, xa, yb, ya, xb = pieces
    r = lax.axis_index("rep")
    piece, nc = own_z.shape
    put(raw, qc, vc, slot, rows_at(r, piece), slice(0, nc), own_z[...])
    left, right = slice(0, nc // 2), slice(nc // 2, nc)
    for cols, group in ((left, (xa[...], ya[0], ya[1])), (right, (xb[0], yb[...], xb[1]))):
        for m, w in enumerate(group):
            put(raw, qc, vc, slot, rows_at(r ^ (m + 1), piece), cols, w)

def send(qc, vc, qc_h, vc_h, slot, here, sem, at):
    moves = [
        pltpu.make_async_copy(qc.at[slot], qc_h.at[here, :], sem.at[at]),
        pltpu.make_async_copy(vc.at[slot], vc_h.at[here, :], sem.at[at + 1]),
    ]
    for c in moves:
        c.start()
    return moves

def final_body(nt, *refs):
    fac, ratio, tot, tot_in, wq, wv = refs[:6]
    near, far = refs[6:8], refs[8:-14]
    qd_h, vd_h, qm_h, vm_h, qc_h, vc_h, raw, qd, vd, qm, vm, qc, vc, sem = refs[-14:]
    f = lax.axis_index("fs")
    dl, nq, nv = wq.shape[0], wq.shape[1], wv.shape[1]
    scale = scales(fac, tot, tot_in, nq, nv, nt)
    stores = []
    for k in range(2 + len(far) // 5):
        step_rows(fac, ratio, raw, rows_at(f ^ k, dl), nq, scale)
        if k == 0:
            qd[...] = raw[:, :nq]
            vd[...] = raw[:, nq:]
            qm[...] = wq[...] - RATE * raw[:, :nq]
            vm[...] = wv[...] - RATE * raw[:, nq:]
            put(raw, qc, vc, 0, slice(None), slice(0, nq), wq[...].astype(BF))
            put(raw, qc, vc, 0, slice(None), slice(nq, nq + nv), wv[...].astype(BF))
            stores += [
                pltpu.make_async_copy(qd, qd_h, sem.at[0]),
                pltpu.make_async_copy(vd, vd_h, sem.at[1]),
                pltpu.make_async_copy(qm, qm_h, sem.at[2]),
                pltpu.make_async_copy(vm, vm_h, sem.at[3]),
            ]
            for c in stores:
                c.start()
        elif k == 1:
            put(raw, qc, vc, 1, slice(0, dl // 2), slice(0, nq + nv), near[0][...])
            put(raw, qc, vc, 1, slice(dl // 2, dl), slice(0, nq + nv), near[1][...])
        else:
            put_far(raw, qc, vc, k, far[5 * (k - 2) : 5 * (k - 1)])
        stores += send(qc, vc, qc_h, vc_h, k, rows_at(f ^ k, dl), sem, 4 + 2 * k)
    for c in stores:
        c.wait()

def last_body(k, nt, *refs):
    fac, ratio, tot, tot_in = refs[:4]
    far, (qc_h, vc_h, raw, qc, vc, sem) = refs[4:9], refs[11:]
    f = lax.axis_index("fs")
    dl, nq, nv = qc.shape[1], qc.shape[2], vc.shape[2]
    here = rows_at(f ^ k, dl)
    step_rows(fac, ratio, raw, here, nq, scales(fac, tot, tot_in, nq, nv, nt))
    put_far(raw, qc, vc, 0, far)
    for c in send(qc, vc, qc_h, vc_h, 0, here, sem, 0):
        c.wait()

def exchange(nf, nr, nt, xs, cq, cv, wq, wv, fq, fv, q1, q2, v1, v2):
    S = jax.ShapeDtypeStruct
    dl, rank = fq.shape
    nq, nv = cq.shape[1], cv.shape[1]
    nc = nq + nv
    half = nc // 2
    d = nf * dl
    piece = dl // nr
    tokens = xs.shape[0]

    (start,) = call(functools.partial(first_body, nr), [S((piece, rank), BF)], 2, [pltpu.SemaphoreType.DMA], limit=60, in_specs=[ANY] * 2)(fq, fv)
    zs = [swap(start, "fs", nf, k) for k in range(1, nf)]
    stacked = jnp.stack(zs)
    mine = [stacked] + [swap(stacked, "rep", nr, j) for j in range(1, nr)]
    other = [swap(m, "tp", nt, 1) for m in mine]

    quarter, low, high = call(
        functools.partial(pack_body, nr),
        [S((piece, nc), BF)] + [S((dl // 2, nc), BF)] * 2,
        2,
        [pltpu.VMEM((dl, nq), F32), pltpu.VMEM((dl, nv), F32), pltpu.SemaphoreType.DMA((2,))],
        in_specs=[ANY] * 2,
        limit=12,
    )(wq, wv)
    near = [swap(low, "fs", nf, 1), swap(high, "fs", nf, 1)]
    far = []
    for k in range(2, nf):
        own_z = swap(quarter, "fs", nf, k)
        fa, fb = own_z[:, :half], own_z[:, half:]
        xa = swap(fa, "rep", nr, 1)
        yb = swap(fb, "rep", nr, 2)
        ya = swap(jnp.stack([fa, xa]), "rep", nr, 2)
        xb = swap(jnp.stack([fb, yb]), "rep", nr, 1)
        far += [own_z, xa, yb, ya, xb]

    cot = jnp.concatenate([cq, cv], axis=1)
    h = rank // nr
    *parts, fac = call(
        functools.partial(project_body, nf, nr, nq),
        [S((h, nc), BF)] * nr + [S((2, d, rank), BF)],
        4 + 2 * nr,
        [pltpu.VMEM((rank, nc), BF)],
        limit=24,
        flops=2 * tokens * (d * 2 * rank + rank * nc),
        nbytes=2 * (tokens * (d + nc) + 4 * d * rank),
    )(xs, fq, fv, cot, *mine, *other)
    (gram,) = call(gram_body, [S((2, rank, rank), F32)], 1, flops=4 * d * rank * rank, nbytes=4 * d * rank)(fac)

    got = [parts[0]] + [swap(parts[j], "rep", nr, j) for j in range(1, nr)]
    g = h // nf
    own, *rest = call(
        functools.partial(plane_sum_body, nf, nr),
        [S((g, nc), F32)] + [S((g, nc), BF)] * (nf - 1),
        nr,
        [pltpu.VMEM((h, nc), F32)],
    )(*got)
    got = [own] + [swap(rest[k - 1], "fs", nf, k) for k in range(1, nf)]
    (proj,) = call(functools.partial(line_sum_body, nf), [S((g, nc), BF)], nf)(*got)
    got = [proj] + [swap(proj, "fs", nf, k) for k in range(1, nf)]
    q1n, q2n, v1n, v2n, ratio = call(
        functools.partial(moments_body, nf, nq),
        [S((h, nq), F32)] * 2 + [S((h, nv), F32)] * 2 + [S((h, nc), BF)],
        nf + 4,
        [pltpu.VMEM((h, nc), F32)],
    )(*got, q1, q2, v1, v2)
    got = [ratio] + [swap(ratio, "rep", nr, j) for j in range(1, nr)]
    ratios, total = call(
        functools.partial(total_body, nr, nq), [S((rank, nc), BF), S((16, 128), F32)], nr + 1, limit=12
    )(*got, gram)
    total_in = swap(total, "tp", nt, 1)
    given = (fac, ratios, total, total_in)
    qd, vd, qm, vm, qc, vc = call(
        functools.partial(final_body, nt),
        [S((dl, nq), F32), S((dl, nv), F32)] * 2 + [S((d, nq), BF), S((d, nv), BF)],
        8 + 5 * (nf - 3),
        [
            pltpu.VMEM((dl, nc), F32),
            pltpu.VMEM((dl, nq), F32),
            pltpu.VMEM((dl, nv), F32),
            pltpu.VMEM((dl, nq), F32),
            pltpu.VMEM((dl, nv), F32),
            pltpu.VMEM((nf - 1, dl, nq), BF),
            pltpu.VMEM((nf - 1, dl, nv), BF),
            pltpu.SemaphoreType.DMA((4 + 2 * nf,)),
        ],
        limit=30,
        out_specs=[ANY] * 6,
        flops=2 * d * rank * nc,
        nbytes=2 * d * nc * 2 + 12 * dl * nc,
    )(*given, wq, wv, *near, *far[:-5])
    qc, vc = call(
        functools.partial(last_body, nf - 1, nt),
        [S((d, nq), BF), S((d, nv), BF)],
        11,
        [
            pltpu.VMEM((dl, nc), F32),
            pltpu.VMEM((1, dl, nq), BF),
            pltpu.VMEM((1, dl, nv), BF),
            pltpu.SemaphoreType.DMA((2,)),
        ],
        limit=16,
        in_specs=[VMEM] * 9 + [ANY] * 2,
        out_specs=[ANY] * 2,
        flops=2 * dl * rank * nc,
        nbytes=2 * dl * nc * 2,
        aliases={9: 0, 10: 1},
    )(*given, *far[-5:], qc, vc)
    return qd, vd, qm, vm, qc, vc, q1n, q2n, v1n, v2n

def moments(projected, first, second):
    first_new = BETA_ONE * first + (1.0 - BETA_ONE) * projected
    second_new = BETA_TWO * second + (1.0 - BETA_TWO) * projected * projected
    ratio = first_new / (jnp.sqrt(second_new) + EPS_RATIO)
    return (first_new, second_new, ratio)

def collective(nf, nt, xs, cq, cv, wq, wv, fq, fv, q1, q2, v1, v2):
    dims = (((0,), (0,)), ((), ()))
    highest = lax.Precision.HIGHEST

    def one(cot, weight, factor, first, second):
        grad = lax.dot_general(xs, cot, dims, preferred_element_type=F32)
        whole = lax.all_gather(factor, "fs", axis=0, tiled=True).astype(F32)
        proj = jnp.dot(whole.T, grad, precision=highest)
        proj = lax.psum_scatter(proj.astype(BF), "rep", scatter_dimension=0, tiled=True).astype(F32)
        first_new, second_new, ratio = moments(lax.psum(proj, "fs"), first, second)
        ratio = lax.all_gather(ratio, "rep", axis=0, tiled=True)
        raw = jnp.dot(factor.astype(F32), ratio, precision=highest)
        total = lax.psum(jnp.sum(raw * raw), ("fs", "tp"))
        size = raw.size * nf * nt
        direction = raw * lax.rsqrt(total / size + EPS_NORM)
        master = weight - RATE * direction
        copy = lax.all_gather(master.astype(BF), "fs", axis=0, tiled=True)
        return direction, master, first_new, second_new, copy

    qd, qm, q1n, q2n, qc = one(cq, wq, fq, q1, q2)
    vd, vm, v1n, v2n, vc = one(cv, wv, fv, v1, v2)
    return qd, vd, qm, vm, q1n, q2n, v1n, v2n, qc, vc

def local(nf, nr, nt, *args):
    rank = args[5].shape[1]
    if not square(nf, nr, nt) or rank % (nf * nr * TILE):
        return collective(nf, nt, *args)
    qd, vd, qm, vm, qc, vc, *new = exchange(nf, nr, nt, *args)
    return qd, vd, qm, vm, *new, qc, vc

def square(nf, nr, nt):
    return (nf, nr, nt) == (4, 2 * 2, 2)

def solution(mesh):
    placed = (
        P(("fs", "rep"), None),
        P(("fs", "rep"), "tp"),
        P(("fs", "rep"), "tp"),
        P("fs", "tp"),
        P("fs", "tp"),
        P("fs", None),
        P("fs", None),
        P("rep", "tp"),
        P("rep", "tp"),
        P("rep", "tp"),
        P("rep", "tp"),
    )
    return jax.shard_map(
        functools.partial(local, mesh.shape["fs"], mesh.shape["rep"], mesh.shape["tp"]),
        mesh=mesh,
        in_specs=placed,
        out_specs=(P("fs", "tp"),) * 4 + (P("rep", "tp"),) * 4 + (P(None, "tp"),) * 2,
        check_vma=False,
    )
```

```python
import functools

import jax
import jax.numpy as jnp
from jax import lax
from jax.experimental import pallas as pl
from jax.experimental.pallas import tpu as pltpu
from jax.sharding import PartitionSpec as P


BETA_ONE = 0.8
BETA_TWO = 0.9
EPS_RATIO = 1e-08
EPS_NORM = 1e-06
RATE = 0.02


BF = jnp.bfloat16
F32 = jnp.float32
VMEM = pl.BlockSpec(memory_space=pltpu.VMEM)
ANY = pl.BlockSpec(memory_space=pltpu.HBM)
TILE = 16
EARLY = 5

def swap(x, axis, n, k):
    return lax.ppermute(x, axis, [(i, i ^ k) for i in range(n)])

def rows_at(block, height):
    return pl.ds(pl.multiple_of(block * height, height), height)

def call(body, outs, n_in, scratch=(), limit=8, flops=0, nbytes=0, in_specs=None, out_specs=None, aliases=None):
    return pl.pallas_call(
        body,
        out_shape=outs,
        in_specs=in_specs or [VMEM] * n_in,
        out_specs=out_specs or [VMEM] * len(outs),
        scratch_shapes=list(scratch),
        input_output_aliases=aliases or {},
        compiler_params=pltpu.CompilerParams(vmem_limit_bytes=limit << 20),
        cost_estimate=pl.CostEstimate(flops=flops, bytes_accessed=nbytes, transcendentals=0),
    )

def pack_body(wq, wv, low, high):
    nq = wq.shape[1]
    for ref, here in ((low, slice(0, low.shape[0])), (high, slice(low.shape[0], wq.shape[0]))):
        ref[:, :nq] = wq[here, :].astype(BF)
        ref[:, nq:] = wv[here, :].astype(BF)


def collect(nf, nr, out, pieces):
    f, r = lax.axis_index("fs"), lax.axis_index("rep")
    height = pieces[0].shape[1]
    for k in range(1, nf):
        for j in range(nr):
            out[rows_at((f ^ k) * nr + (r ^ j), height), :] = pieces[j][k - 1]


def lift_body(nf, nr, x, fq, fv, *refs):
    pieces, (y, fac) = refs[:nr], refs[nr:]
    own = rows_at(lax.axis_index("fs"), fq.shape[0])
    for s, ref in enumerate((fq, fv)):

        @pl.when(lax.axis_index("tp") == s)
        def _():
            fac[own, :] = ref[...]

    collect(nf, nr, fac, pieces)
    y[...] = jnp.dot(x[...], fac[...], preferred_element_type=F32).astype(BF)


def project_body(nf, nr, nq, x, fq, fv, cot, y_mine, mine, *refs):
    pieces, outs, (fac, y, part) = refs[:nr], refs[nr : 2 * nr], refs[2 * nr :]
    f, r, t = lax.axis_index("fs"), lax.axis_index("rep"), lax.axis_index("tp")
    own = rows_at(f, fq.shape[0])
    other = fac.at[1 - t]
    for s, ref in enumerate((fq, fv)):

        @pl.when(t != s)
        def _():
            other[own, :] = ref[...]

    collect(nf, nr, other, pieces)
    y[1 - t] = jnp.dot(x[...], other[...], preferred_element_type=F32).astype(BF)
    y[t] = y_mine[...]
    fac[t] = mine[...]
    dims = (((0,), (0,)), ((), ()))
    for s, cols in ((0, slice(None, nq)), (1, slice(nq, None))):
        part[:, cols] = lax.dot_general(y[s], cot[:, cols], dims, preferred_element_type=F32).astype(BF)
    h = part.shape[0] // nr
    for j in range(nr):
        outs[j][...] = part[rows_at(r ^ j, h), :]


def plane_sum_body(nf, nr, *refs):
    ins, own, rest, acc = refs[:nr], refs[nr], refs[nr + 1 : nr + nf], refs[nr + nf]
    f = lax.axis_index("fs")
    total = ins[0][...].astype(F32)
    for ref in ins[1:]:
        total += ref[...].astype(F32)
    acc[...] = total
    h = acc.shape[0] // nf
    own[...] = acc[rows_at(f, h), :]
    for k in range(1, nf):
        rest[k - 1][...] = acc[rows_at(f ^ k, h), :].astype(BF)

def line_sum_body(nf, *refs):
    total = refs[0][...]
    for ref in refs[1:nf]:
        total += ref[...].astype(F32)
    refs[nf][...] = total.astype(BF)

def moments_body(nf, nq, *refs):
    ins = refs[:nf]
    q1, q2, v1, v2 = refs[nf : nf + 4]
    q1n, q2n, v1n, v2n, ratio, proj = refs[nf + 4 :]
    f = lax.axis_index("fs")
    h = ins[0].shape[0]
    for k in range(nf):
        proj[rows_at(f ^ k, h), :] = ins[k][...].astype(F32)
    for cols, first, second, fo, so in (
        (slice(None, nq), q1, q2, q1n, q2n),
        (slice(nq, None), v1, v2, v1n, v2n),
    ):
        p = proj[:, cols]
        fn = BETA_ONE * first[...] + (1.0 - BETA_ONE) * p
        sn = BETA_TWO * second[...] + (1.0 - BETA_TWO) * p * p
        fo[...] = fn
        so[...] = sn
        ratio[:, cols] = (fn / (jnp.sqrt(sn) + EPS_RATIO)).astype(BF)

def gram_body(fac, out):
    dims = (((0,), (0,)), ((), ()))
    for s in range(2):
        out[s] = lax.dot_general(fac[s], fac[s], dims, preferred_element_type=F32)

def total_body(nr, nq, *refs):
    ins, gram, ratio, total = refs[:nr], refs[nr], refs[nr + 1], refs[nr + 2]
    r = lax.axis_index("rep")
    h = ins[0].shape[0]
    for j in range(nr):
        ratio[rows_at(r ^ j, h), :] = ins[j][...]
    for s, cols in ((0, slice(None, nq)), (1, slice(nq, None))):
        z = ratio[:, cols]
        g = gram[s]
        acc = None
        for _ in range(3):
            high = g.astype(BF)
            g = g - high.astype(F32)
            term = jnp.dot(high, z, preferred_element_type=F32)
            acc = term if acc is None else acc + term
        total[rows_at(s, 8), :] = jnp.broadcast_to(jnp.sum(acc * z.astype(F32), keepdims=True), (8, 128))

def scales(fac, tot, tot_in, nq, nv, nt):
    both = tot[...] + tot_in[...]
    d = fac.shape[1]
    return (
        lax.rsqrt(both[0:1, 0:1] / (d * nq * nt) + EPS_NORM),
        lax.rsqrt(both[8:9, 0:1] / (d * nv * nt) + EPS_NORM),
    )


def step_rows(fac, ratio, raw, here, nq, scale=(1.0, 1.0)):
    for s, cols in ((0, slice(None, nq)), (1, slice(nq, None))):
        raw[:, cols] = jnp.dot(fac[s, here, :], ratio[:, cols], preferred_element_type=F32) * scale[s]


def raw_body(nq, fac, ratio, raw):
    step_rows(fac, ratio, raw, rows_at(lax.axis_index("fs"), raw.shape[0]), nq)


def put(raw, qc, vc, slot, here, cols, w):
    nq = qc.shape[2]
    value = (w.astype(F32) - RATE * raw[here, cols]).astype(BF)
    split = min(max(nq - cols.start, 0), cols.stop - cols.start)
    if split:
        qc[slot, here, cols.start : cols.start + split] = value[:, :split]
    if split < cols.stop - cols.start:
        vc[slot, here, cols.start + split - nq : cols.stop - nq] = value[:, split:]

def put_far(raw, qc, vc, slot, pieces):
    own_z, xa, yb, ya, xb = pieces
    r = lax.axis_index("rep")
    piece, nc = own_z.shape
    put(raw, qc, vc, slot, rows_at(r, piece), slice(0, nc), own_z[...])
    left, right = slice(0, nc // 2), slice(nc // 2, nc)
    for cols, group in ((left, (xa[...], ya[0], ya[1])), (right, (xb[0], yb[...], xb[1]))):
        for m, w in enumerate(group):
            put(raw, qc, vc, slot, rows_at(r ^ (m + 1), piece), cols, w)

def send(qc, vc, qc_h, vc_h, slot, here, sem, at):
    moves = [
        pltpu.make_async_copy(qc.at[slot], qc_h.at[here, :], sem.at[at]),
        pltpu.make_async_copy(vc.at[slot], vc_h.at[here, :], sem.at[at + 1]),
    ]
    for c in moves:
        c.start()
    return moves

def final_body(nt, *refs):
    fac, ratio, tot, tot_in, raw_own, wq, wv = refs[:7]
    far = refs[7:-15]
    qd_h, vd_h, qm_h, vm_h, qc_h, vc_h, raw_last, raw, qd, vd, qm, vm, qc, vc, sem = refs[-15:]
    f = lax.axis_index("fs")
    dl, nq, nv = wq.shape[0], wq.shape[1], wv.shape[1]
    scale = scales(fac, tot, tot_in, nq, nv, nt)
    stores = []
    for n, (here, w, dr, ms) in enumerate(((slice(0, nq), wq, qd, qm), (slice(nq, nq + nv), wv, vd, vm))):
        dr[...] = raw_own[:, here] * scale[n]
        stores.append(pltpu.make_async_copy(dr, (qd_h, vd_h)[n], sem.at[n]))
        stores[-1].start()
        ms[...] = w[...] - RATE * dr[...]
        stores.append(pltpu.make_async_copy(ms, (qm_h, vm_h)[n], sem.at[2 + n]))
        stores[-1].start()
        put_own(dr, (qc, vc)[n], w)
    stores += send(qc, vc, qc_h, vc_h, 0, rows_at(f, dl), sem, 4)
    step_rows(fac, ratio, raw, rows_at(f ^ 2, dl), nq, scale)
    put_far(raw, qc, vc, 1, far)
    stores += send(qc, vc, qc_h, vc_h, 1, rows_at(f ^ 2, dl), sem, 6)
    for n, k in enumerate((1, 3)):
        step_rows(fac, ratio, raw_last.at[n], rows_at(f ^ k, dl), nq, scale)
    for c in stores:
        c.wait()


def put_own(step, copy, w):
    copy[0] = (w[...].astype(BF).astype(F32) - RATE * step[...]).astype(BF)


def last_body(raw, *refs):
    near, far, (qc_h, vc_h, qc, vc, sem) = refs[:2], refs[2:7], refs[9:]
    f = lax.axis_index("fs")
    dl, whole = qc.shape[1], slice(0, raw.shape[2])
    cut = near[0].shape[0]
    put(raw.at[0], qc, vc, 0, slice(0, cut), whole, near[0][...])
    put(raw.at[0], qc, vc, 0, slice(cut, dl), whole, near[1][...])
    stores = send(qc, vc, qc_h, vc_h, 0, rows_at(f ^ 1, dl), sem, 0)
    put_far(raw.at[1], qc, vc, 1, far)
    stores += send(qc, vc, qc_h, vc_h, 1, rows_at(f ^ 3, dl), sem, 2)
    for c in stores:
        c.wait()


def exchange(nf, nr, nt, xs, cq, cv, wq, wv, fq, fv, q1, q2, v1, v2):
    S = jax.ShapeDtypeStruct
    dl, rank = fq.shape
    nq, nv = cq.shape[1], cv.shape[1]
    nc = nq + nv
    half = nc // 2
    d = nf * dl
    piece = dl // nr
    tokens = xs.shape[0]

    mine_at = lax.axis_index("rep") * piece
    start = jnp.where(
        lax.axis_index("tp") == 0,
        lax.dynamic_slice_in_dim(fq, mine_at, piece, 0),
        lax.dynamic_slice_in_dim(fv, mine_at, piece, 0),
    )
    zs = [swap(start, "fs", nf, k) for k in range(1, nf)]
    stacked = jnp.stack(zs)
    mine = [stacked] + [swap(stacked, "rep", nr, j) for j in range(1, nr)]
    other = [swap(m, "tp", nt, 1) for m in mine]

    quarter = jnp.concatenate(
        [lax.dynamic_slice_in_dim(w, mine_at, piece, 0).astype(BF) for w in (wq, wv)], axis=1
    )
    early = EARLY * dl // 16
    low, high = call(pack_body, [S((early, nc), BF), S((dl - early, nc), BF)], 2, limit=12)(wq, wv)
    near = [swap(low, "fs", nf, 1), swap(high, "fs", nf, 1)]
    far = []
    own_z = quarter
    for k in range(2, nf):
        own_z = swap(own_z, "fs", nf, 2 if k == 2 else 1)
        fa, fb = own_z[:, :half], own_z[:, half:]
        xa = swap(fa, "rep", nr, 1)
        yb = swap(fb, "rep", nr, 2)
        ya = swap(jnp.stack([fa, xa]), "rep", nr, 2)
        xb = swap(jnp.stack([fb, yb]), "rep", nr, 1)
        far += [own_z, xa, yb, ya, xb]

    cot = jnp.concatenate([cq, cv], axis=1)
    h = rank // nr
    y_mine, fac_mine = call(
        functools.partial(lift_body, nf, nr),
        [S((tokens, rank), BF), S((d, rank), BF)],
        3 + nr,
        limit=12,
        flops=2 * tokens * d * rank,
        nbytes=2 * (tokens * d + 2 * d * rank),
    )(xs, fq, fv, *mine)
    *parts, fac = call(
        functools.partial(project_body, nf, nr, nq),
        [S((h, nc), BF)] * nr + [S((2, d, rank), BF)],
        6 + nr,
        [pltpu.VMEM((2, tokens, rank), BF), pltpu.VMEM((rank, nc), BF)],
        limit=24,
        flops=2 * tokens * (d * rank + rank * nc),
        nbytes=2 * (tokens * (d + nc) + 4 * d * rank),
    )(xs, fq, fv, cot, y_mine, fac_mine, *other)
    (gram,) = call(gram_body, [S((2, rank, rank), F32)], 1, flops=4 * d * rank * rank, nbytes=4 * d * rank)(fac)

    got = [parts[0]] + [swap(parts[j], "rep", nr, j) for j in range(1, nr)]
    g = h // nf
    own, *rest = call(
        functools.partial(plane_sum_body, nf, nr),
        [S((g, nc), F32)] + [S((g, nc), BF)] * (nf - 1),
        nr,
        [pltpu.VMEM((h, nc), F32)],
    )(*got)
    got = [own] + [swap(rest[k - 1], "fs", nf, k) for k in range(1, nf)]
    (proj,) = call(functools.partial(line_sum_body, nf), [S((g, nc), BF)], nf)(*got)
    got = [proj] + [swap(proj, "fs", nf, k) for k in range(1, nf)]
    q1n, q2n, v1n, v2n, ratio = call(
        functools.partial(moments_body, nf, nq),
        [S((h, nq), F32)] * 2 + [S((h, nv), F32)] * 2 + [S((h, nc), BF)],
        nf + 4,
        [pltpu.VMEM((h, nc), F32)],
    )(*got, q1, q2, v1, v2)
    got = [ratio] + [swap(ratio, "rep", nr, j) for j in range(1, nr)]
    ratios, total = call(
        functools.partial(total_body, nr, nq), [S((rank, nc), BF), S((16, 128), F32)], nr + 1, limit=12
    )(*got, gram)
    total_in = swap(total, "tp", nt, 1)
    (raw_own,) = call(
        functools.partial(raw_body, nq),
        [S((dl, nc), F32)],
        2,
        limit=12,
        flops=2 * dl * rank * nc,
        nbytes=2 * (2 * d * rank + rank * nc) + 4 * dl * nc,
    )(fac, ratios)
    qd, vd, qm, vm, qc, vc, raw_last = call(
        functools.partial(final_body, nt),
        [S((dl, nq), F32), S((dl, nv), F32)] * 2 + [S((d, nq), BF), S((d, nv), BF), S((2, dl, nc), F32)],
        12,
        [
            pltpu.VMEM((dl, nc), F32),
            pltpu.VMEM((dl, nq), F32),
            pltpu.VMEM((dl, nv), F32),
            pltpu.VMEM((dl, nq), F32),
            pltpu.VMEM((dl, nv), F32),
            pltpu.VMEM((2, dl, nq), BF),
            pltpu.VMEM((2, dl, nv), BF),
            pltpu.SemaphoreType.DMA((8,)),
        ],
        limit=30,
        out_specs=[ANY] * 6 + [VMEM],
        flops=2 * d * rank * nc,
        nbytes=2 * d * nc * 2 + 12 * dl * nc,
    )(fac, ratios, total, total_in, raw_own, wq, wv, *far[:5])
    qc, vc = call(
        last_body,
        [S((d, nq), BF), S((d, nv), BF)],
        10,
        [
            pltpu.VMEM((2, dl, nq), BF),
            pltpu.VMEM((2, dl, nv), BF),
            pltpu.SemaphoreType.DMA((4,)),
        ],
        limit=16,
        in_specs=[VMEM] * 8 + [ANY] * 2,
        out_specs=[ANY] * 2,
        flops=4 * dl * nc,
        nbytes=8 * dl * nc,
        aliases={8: 0, 9: 1},
    )(raw_last, *near, *far[5:], qc, vc)
    return qd, vd, qm, vm, qc, vc, q1n, q2n, v1n, v2n


def moments(projected, first, second):
    first_new = BETA_ONE * first + (1.0 - BETA_ONE) * projected
    second_new = BETA_TWO * second + (1.0 - BETA_TWO) * projected * projected
    ratio = first_new / (jnp.sqrt(second_new) + EPS_RATIO)
    return (first_new, second_new, ratio)

def collective(nf, nt, xs, cq, cv, wq, wv, fq, fv, q1, q2, v1, v2):
    dims = (((0,), (0,)), ((), ()))
    highest = lax.Precision.HIGHEST

    def one(cot, weight, factor, first, second):
        grad = lax.dot_general(xs, cot, dims, preferred_element_type=F32)
        whole = lax.all_gather(factor, "fs", axis=0, tiled=True).astype(F32)
        proj = jnp.dot(whole.T, grad, precision=highest)
        proj = lax.psum_scatter(proj.astype(BF), "rep", scatter_dimension=0, tiled=True).astype(F32)
        first_new, second_new, ratio = moments(lax.psum(proj, "fs"), first, second)
        ratio = lax.all_gather(ratio, "rep", axis=0, tiled=True)
        raw = jnp.dot(factor.astype(F32), ratio, precision=highest)
        total = lax.psum(jnp.sum(raw * raw), ("fs", "tp"))
        size = raw.size * nf * nt
        direction = raw * lax.rsqrt(total / size + EPS_NORM)
        master = weight - RATE * direction
        copy = lax.all_gather(master.astype(BF), "fs", axis=0, tiled=True)
        return direction, master, first_new, second_new, copy

    qd, qm, q1n, q2n, qc = one(cq, wq, fq, q1, q2)
    vd, vm, v1n, v2n, vc = one(cv, wv, fv, v1, v2)
    return qd, vd, qm, vm, q1n, q2n, v1n, v2n, qc, vc

def local(nf, nr, nt, *args):
    rank = args[5].shape[1]
    if not square(nf, nr, nt) or rank % (nf * nr * TILE):
        return collective(nf, nt, *args)
    qd, vd, qm, vm, qc, vc, *new = exchange(nf, nr, nt, *args)
    return qd, vd, qm, vm, *new, qc, vc

def square(nf, nr, nt):
    return (nf, nr, nt) == (4, 2 * 2, 2)

def solution(mesh):
    placed = (
        P(("fs", "rep"), None),
        P(("fs", "rep"), "tp"),
        P(("fs", "rep"), "tp"),
        P("fs", "tp"),
        P("fs", "tp"),
        P("fs", None),
        P("fs", None),
        P("rep", "tp"),
        P("rep", "tp"),
        P("rep", "tp"),
        P("rep", "tp"),
    )
    return jax.shard_map(
        functools.partial(local, mesh.shape["fs"], mesh.shape["rep"], mesh.shape["tp"]),
        mesh=mesh,
        in_specs=placed,
        out_specs=(P("fs", "tp"),) * 4 + (P("rep", "tp"),) * 4 + (P(None, "tp"),) * 2,
        check_vma=False,
    )
```

```python
import functools

import jax
import jax.numpy as jnp
from jax import lax
from jax.experimental import pallas as pl
from jax.experimental.pallas import tpu as pltpu
from jax.sharding import PartitionSpec as P


BETA_ONE = 0.8
BETA_TWO = 0.9
EPS_RATIO = 1e-08
EPS_NORM = 1e-06
RATE = 0.02


BF = jnp.bfloat16
F32 = jnp.float32
VMEM = pl.BlockSpec(memory_space=pltpu.VMEM)
ANY = pl.BlockSpec(memory_space=pltpu.HBM)
TILE = 16
EARLY = 12

def swap(x, axis, n, k):
    return lax.ppermute(x, axis, [(i, i ^ k) for i in range(n)])

def rows_at(block, height):
    return pl.ds(pl.multiple_of(block * height, height), height)

def call(body, outs, n_in, scratch=(), limit=8, flops=0, nbytes=0, in_specs=None, out_specs=None, aliases=None):
    return pl.pallas_call(
        body,
        out_shape=outs,
        in_specs=in_specs or [VMEM] * n_in,
        out_specs=out_specs or [VMEM] * len(outs),
        scratch_shapes=list(scratch),
        input_output_aliases=aliases or {},
        compiler_params=pltpu.CompilerParams(vmem_limit_bytes=limit << 20),
        cost_estimate=pl.CostEstimate(flops=flops, bytes_accessed=nbytes, transcendentals=0),
    )

def pack_body(wq, wv, low, high):
    nq = wq.shape[1]
    for ref, here in ((low, slice(0, low.shape[0])), (high, slice(low.shape[0], wq.shape[0]))):
        ref[:, :nq] = wq[here, :].astype(BF)
        ref[:, nq:] = wv[here, :].astype(BF)


def collect(nf, nr, out, pieces):
    f, r = lax.axis_index("fs"), lax.axis_index("rep")
    height = pieces[0].shape[1]
    for k in range(1, nf):
        for j in range(nr):
            out[rows_at((f ^ k) * nr + (r ^ j), height), :] = pieces[j][k - 1]


def lift_body(nf, nr, x, fq, fv, *refs):
    pieces, (y, fac) = refs[:nr], refs[nr:]
    own = rows_at(lax.axis_index("fs"), fq.shape[0])
    for s, ref in enumerate((fq, fv)):

        @pl.when(lax.axis_index("tp") == s)
        def _():
            fac[own, :] = ref[...]

    collect(nf, nr, fac, pieces)
    y[...] = jnp.dot(x[...], fac[...], preferred_element_type=F32).astype(BF)


def project_body(nf, nr, nq, x, fq, fv, cot, y_mine, mine, *refs):
    pieces, outs, (fac, y, part) = refs[:nr], refs[nr : 2 * nr], refs[2 * nr :]
    f, r, t = lax.axis_index("fs"), lax.axis_index("rep"), lax.axis_index("tp")
    own = rows_at(f, fq.shape[0])
    other = fac.at[1 - t]
    for s, ref in enumerate((fq, fv)):

        @pl.when(t != s)
        def _():
            other[own, :] = ref[...]

    collect(nf, nr, other, pieces)
    y[1 - t] = jnp.dot(x[...], other[...], preferred_element_type=F32).astype(BF)
    y[t] = y_mine[...]
    fac[t] = mine[...]
    dims = (((0,), (0,)), ((), ()))
    for s, cols in ((0, slice(None, nq)), (1, slice(nq, None))):
        part[:, cols] = lax.dot_general(y[s], cot[:, cols], dims, preferred_element_type=F32).astype(BF)
    h = part.shape[0] // nr
    for j in range(nr):
        outs[j][...] = part[rows_at(r ^ j, h), :]


def plane_sum_body(nf, nr, *refs):
    ins, own, rest, acc = refs[:nr], refs[nr], refs[nr + 1 : nr + nf], refs[nr + nf]
    f = lax.axis_index("fs")
    total = ins[0][...].astype(F32)
    for ref in ins[1:]:
        total += ref[...].astype(F32)
    acc[...] = total
    h = acc.shape[0] // nf
    own[...] = acc[rows_at(f, h), :]
    for k in range(1, nf):
        rest[k - 1][...] = acc[rows_at(f ^ k, h), :].astype(BF)

def line_sum_body(nf, *refs):
    total = refs[0][...]
    for ref in refs[1:nf]:
        total += ref[...].astype(F32)
    refs[nf][...] = total.astype(BF)

def advance(p, first, second):
    first_new = BETA_ONE * first[...] + (1.0 - BETA_ONE) * p
    return first_new, BETA_TWO * second[...] + (1.0 - BETA_TWO) * p * p


def moments_body(nf, nq, *refs):
    ins, (q1, q2, v1, v2, ratio, proj) = refs[:nf], refs[nf:]
    f = lax.axis_index("fs")
    h = ins[0].shape[0]
    for k in range(nf):
        proj[rows_at(f ^ k, h), :] = ins[k][...].astype(F32)
    for cols, first, second in ((slice(None, nq), q1, q2), (slice(nq, None), v1, v2)):
        fn, sn = advance(proj[:, cols], first, second)
        ratio[:, cols] = (fn / (jnp.sqrt(sn) + EPS_RATIO)).astype(BF)


def state_body(nq, proj, q1, q2, v1, v2, q1n, q2n, v1n, v2n):
    q1n[...], q2n[...] = advance(proj[:, :nq], q1, q2)
    v1n[...], v2n[...] = advance(proj[:, nq:], v1, v2)


def gram_body(fac, out):
    dims = (((0,), (0,)), ((), ()))
    for s in range(2):
        out[s] = lax.dot_general(fac[s], fac[s], dims, preferred_element_type=F32)

def total_body(nr, nq, *refs):
    ins, gram, ratio, total = refs[:nr], refs[nr], refs[nr + 1], refs[nr + 2]
    r = lax.axis_index("rep")
    h = ins[0].shape[0]
    for j in range(nr):
        ratio[rows_at(r ^ j, h), :] = ins[j][...]
    for s, cols in ((0, slice(None, nq)), (1, slice(nq, None))):
        z = ratio[:, cols]
        g = gram[s]
        acc = None
        for _ in range(3):
            high = g.astype(BF)
            g = g - high.astype(F32)
            term = jnp.dot(high, z, preferred_element_type=F32)
            acc = term if acc is None else acc + term
        total[rows_at(s, 8), :] = jnp.broadcast_to(jnp.sum(acc * z.astype(F32), keepdims=True), (8, 128))

def scales(fac, tot, tot_in, nq, nv, nt):
    both = tot[...] + tot_in[...]
    d = fac.shape[1]
    return (
        lax.rsqrt(both[0:1, 0:1] / (d * nq * nt) + EPS_NORM),
        lax.rsqrt(both[8:9, 0:1] / (d * nv * nt) + EPS_NORM),
    )


def step_rows(fac, ratio, raw, here, nq, scale=(1.0, 1.0)):
    for s, cols in ((0, slice(None, nq)), (1, slice(nq, None))):
        raw[:, cols] = jnp.dot(fac[s, here, :], ratio[:, cols], preferred_element_type=F32) * scale[s]


def raw_body(nq, fac, ratio, raw):
    step_rows(fac, ratio, raw, rows_at(lax.axis_index("fs"), raw.shape[0]), nq)


def put(raw, qc, vc, slot, here, cols, w):
    nq = qc.shape[2]
    value = (w.astype(F32) - RATE * raw[here, cols]).astype(BF)
    split = min(max(nq - cols.start, 0), cols.stop - cols.start)
    if split:
        qc[slot, here, cols.start : cols.start + split] = value[:, :split]
    if split < cols.stop - cols.start:
        vc[slot, here, cols.start + split - nq : cols.stop - nq] = value[:, split:]

def put_far(raw, qc, vc, slot, pieces):
    own_z, xa, yb, ya, xb = pieces
    r = lax.axis_index("rep")
    piece, nc = own_z.shape
    put(raw, qc, vc, slot, rows_at(r, piece), slice(0, nc), own_z[...])
    left, right = slice(0, nc // 2), slice(nc // 2, nc)
    for cols, group in ((left, (xa[...], ya[0], ya[1])), (right, (xb[0], yb[...], xb[1]))):
        for m, w in enumerate(group):
            put(raw, qc, vc, slot, rows_at(r ^ (m + 1), piece), cols, w)

def send(qc, vc, qc_h, vc_h, slot, here, sem, at):
    moves = [
        pltpu.make_async_copy(qc.at[slot], qc_h.at[here, :], sem.at[at]),
        pltpu.make_async_copy(vc.at[slot], vc_h.at[here, :], sem.at[at + 1]),
    ]
    for c in moves:
        c.start()
    return moves

def final_body(nt, *refs):
    fac, ratio, tot, tot_in, raw_own, wq, wv = refs[:7]
    far = refs[7:-15]
    qd_h, vd_h, qm_h, vm_h, qc_h, vc_h, raw_last, raw, qd, vd, qm, vm, qc, vc, sem = refs[-15:]
    f = lax.axis_index("fs")
    dl, nq, nv = wq.shape[0], wq.shape[1], wv.shape[1]
    scale = scales(fac, tot, tot_in, nq, nv, nt)
    stores = []
    for n, (here, w, dr, ms) in enumerate(((slice(0, nq), wq, qd, qm), (slice(nq, nq + nv), wv, vd, vm))):
        dr[...] = raw_own[:, here] * scale[n]
        stores.append(pltpu.make_async_copy(dr, (qd_h, vd_h)[n], sem.at[n]))
        stores[-1].start()
        ms[...] = w[...] - RATE * dr[...]
        stores.append(pltpu.make_async_copy(ms, (qm_h, vm_h)[n], sem.at[2 + n]))
        stores[-1].start()
        put_own(dr, (qc, vc)[n], w)
    stores += send(qc, vc, qc_h, vc_h, 0, rows_at(f, dl), sem, 4)
    step_rows(fac, ratio, raw, rows_at(f ^ 2, dl), nq, scale)
    put_far(raw, qc, vc, 1, far)
    stores += send(qc, vc, qc_h, vc_h, 1, rows_at(f ^ 2, dl), sem, 6)
    for n, k in enumerate((1, 3)):
        step_rows(fac, ratio, raw_last.at[n], rows_at(f ^ k, dl), nq, scale)
    for c in stores:
        c.wait()


def put_own(step, copy, w):
    copy[0] = (w[...].astype(BF).astype(F32) - RATE * step[...]).astype(BF)


def last_body(raw, *refs):
    near, far, (qc_h, vc_h, qc, vc, sem) = refs[:2], refs[2:7], refs[9:]
    f = lax.axis_index("fs")
    dl, whole = qc.shape[1], slice(0, raw.shape[2])
    cut = near[0].shape[0]
    put(raw.at[0], qc, vc, 0, slice(0, cut), whole, near[0][...])
    put(raw.at[0], qc, vc, 0, slice(cut, dl), whole, near[1][...])
    stores = send(qc, vc, qc_h, vc_h, 0, rows_at(f ^ 1, dl), sem, 0)
    put_far(raw.at[1], qc, vc, 1, far)
    stores += send(qc, vc, qc_h, vc_h, 1, rows_at(f ^ 3, dl), sem, 2)
    for c in stores:
        c.wait()


def exchange(nf, nr, nt, xs, cq, cv, wq, wv, fq, fv, q1, q2, v1, v2):
    S = jax.ShapeDtypeStruct
    dl, rank = fq.shape
    nq, nv = cq.shape[1], cv.shape[1]
    nc = nq + nv
    half = nc // 2
    d = nf * dl
    piece = dl // nr
    tokens = xs.shape[0]

    mine_at = lax.axis_index("rep") * piece
    start = jnp.where(
        lax.axis_index("tp") == 0,
        lax.dynamic_slice_in_dim(fq, mine_at, piece, 0),
        lax.dynamic_slice_in_dim(fv, mine_at, piece, 0),
    )
    zs = [swap(start, "fs", nf, k) for k in range(1, nf)]
    stacked = jnp.stack(zs)
    mine = [stacked] + [swap(stacked, "rep", nr, j) for j in range(1, nr)]
    other = [swap(m, "tp", nt, 1) for m in mine]

    quarter = jnp.concatenate(
        [lax.dynamic_slice_in_dim(w, mine_at, piece, 0).astype(BF) for w in (wq, wv)], axis=1
    )
    early = EARLY * dl // 32
    low, high = call(pack_body, [S((early, nc), BF), S((dl - early, nc), BF)], 2, limit=12)(wq, wv)
    near = [swap(low, "fs", nf, 1), swap(high, "fs", nf, 1)]
    far = []
    own_z = quarter
    for k in range(2, nf):
        own_z = swap(own_z, "fs", nf, 2 if k == 2 else 1)
        fa, fb = own_z[:, :half], own_z[:, half:]
        xa = swap(fa, "rep", nr, 1)
        yb = swap(fb, "rep", nr, 2)
        ya = swap(jnp.stack([fa, xa]), "rep", nr, 2)
        xb = swap(jnp.stack([fb, yb]), "rep", nr, 1)
        far += [own_z, xa, yb, ya, xb]

    cot = jnp.concatenate([cq, cv], axis=1)
    h = rank // nr
    y_mine, fac_mine = call(
        functools.partial(lift_body, nf, nr),
        [S((tokens, rank), BF), S((d, rank), BF)],
        3 + nr,
        limit=12,
        flops=2 * tokens * d * rank,
        nbytes=2 * (tokens * d + 2 * d * rank),
    )(xs, fq, fv, *mine)
    *parts, fac = call(
        functools.partial(project_body, nf, nr, nq),
        [S((h, nc), BF)] * nr + [S((2, d, rank), BF)],
        6 + nr,
        [pltpu.VMEM((2, tokens, rank), BF), pltpu.VMEM((rank, nc), BF)],
        limit=24,
        flops=2 * tokens * (d * rank + rank * nc),
        nbytes=2 * (tokens * (d + nc) + 4 * d * rank),
    )(xs, fq, fv, cot, y_mine, fac_mine, *other)
    (gram,) = call(gram_body, [S((2, rank, rank), F32)], 1, flops=4 * d * rank * rank, nbytes=4 * d * rank)(fac)

    got = [parts[0]] + [swap(parts[j], "rep", nr, j) for j in range(1, nr)]
    g = h // nf
    own, *rest = call(
        functools.partial(plane_sum_body, nf, nr),
        [S((g, nc), F32)] + [S((g, nc), BF)] * (nf - 1),
        nr,
        [pltpu.VMEM((h, nc), F32)],
    )(*got)
    got = [own] + [swap(rest[k - 1], "fs", nf, k) for k in range(1, nf)]
    (proj,) = call(functools.partial(line_sum_body, nf), [S((g, nc), BF)], nf)(*got)
    got = [proj] + [swap(proj, "fs", nf, k) for k in range(1, nf)]
    ratio, proj = call(
        functools.partial(moments_body, nf, nq), [S((h, nc), BF), S((h, nc), F32)], nf + 4
    )(*got, q1, q2, v1, v2)
    q1n, q2n, v1n, v2n = call(
        functools.partial(state_body, nq), [S((h, nq), F32)] * 2 + [S((h, nv), F32)] * 2, 5
    )(proj, q1, q2, v1, v2)
    got = [ratio] + [swap(ratio, "rep", nr, j) for j in range(1, nr)]
    ratios, total = call(
        functools.partial(total_body, nr, nq), [S((rank, nc), BF), S((16, 128), F32)], nr + 1, limit=12
    )(*got, gram)
    total_in = swap(total, "tp", nt, 1)
    (raw_own,) = call(
        functools.partial(raw_body, nq),
        [S((dl, nc), F32)],
        2,
        limit=12,
        flops=2 * dl * rank * nc,
        nbytes=2 * (2 * d * rank + rank * nc) + 4 * dl * nc,
    )(fac, ratios)
    qd, vd, qm, vm, qc, vc, raw_last = call(
        functools.partial(final_body, nt),
        [S((dl, nq), F32), S((dl, nv), F32)] * 2 + [S((d, nq), BF), S((d, nv), BF), S((2, dl, nc), F32)],
        12,
        [
            pltpu.VMEM((dl, nc), F32),
            pltpu.VMEM((dl, nq), F32),
            pltpu.VMEM((dl, nv), F32),
            pltpu.VMEM((dl, nq), F32),
            pltpu.VMEM((dl, nv), F32),
            pltpu.VMEM((2, dl, nq), BF),
            pltpu.VMEM((2, dl, nv), BF),
            pltpu.SemaphoreType.DMA((8,)),
        ],
        limit=30,
        out_specs=[ANY] * 6 + [VMEM],
        flops=2 * d * rank * nc,
        nbytes=2 * d * nc * 2 + 12 * dl * nc,
    )(fac, ratios, total, total_in, raw_own, wq, wv, *far[:5])
    qc, vc = call(
        last_body,
        [S((d, nq), BF), S((d, nv), BF)],
        10,
        [
            pltpu.VMEM((2, dl, nq), BF),
            pltpu.VMEM((2, dl, nv), BF),
            pltpu.SemaphoreType.DMA((4,)),
        ],
        limit=16,
        in_specs=[VMEM] * 8 + [ANY] * 2,
        out_specs=[ANY] * 2,
        flops=4 * dl * nc,
        nbytes=8 * dl * nc,
        aliases={8: 0, 9: 1},
    )(raw_last, *near, *far[5:], qc, vc)
    return qd, vd, qm, vm, qc, vc, q1n, q2n, v1n, v2n


def moments(projected, first, second):
    first_new = BETA_ONE * first + (1.0 - BETA_ONE) * projected
    second_new = BETA_TWO * second + (1.0 - BETA_TWO) * projected * projected
    ratio = first_new / (jnp.sqrt(second_new) + EPS_RATIO)
    return (first_new, second_new, ratio)

def collective(nf, nt, xs, cq, cv, wq, wv, fq, fv, q1, q2, v1, v2):
    dims = (((0,), (0,)), ((), ()))
    highest = lax.Precision.HIGHEST

    def one(cot, weight, factor, first, second):
        grad = lax.dot_general(xs, cot, dims, preferred_element_type=F32)
        whole = lax.all_gather(factor, "fs", axis=0, tiled=True).astype(F32)
        proj = jnp.dot(whole.T, grad, precision=highest)
        proj = lax.psum_scatter(proj.astype(BF), "rep", scatter_dimension=0, tiled=True).astype(F32)
        first_new, second_new, ratio = moments(lax.psum(proj, "fs"), first, second)
        ratio = lax.all_gather(ratio, "rep", axis=0, tiled=True)
        raw = jnp.dot(factor.astype(F32), ratio, precision=highest)
        total = lax.psum(jnp.sum(raw * raw), ("fs", "tp"))
        size = raw.size * nf * nt
        direction = raw * lax.rsqrt(total / size + EPS_NORM)
        master = weight - RATE * direction
        copy = lax.all_gather(master.astype(BF), "fs", axis=0, tiled=True)
        return direction, master, first_new, second_new, copy

    qd, qm, q1n, q2n, qc = one(cq, wq, fq, q1, q2)
    vd, vm, v1n, v2n, vc = one(cv, wv, fv, v1, v2)
    return qd, vd, qm, vm, q1n, q2n, v1n, v2n, qc, vc

def local(nf, nr, nt, *args):
    rank = args[5].shape[1]
    if not square(nf, nr, nt) or rank % (nf * nr * TILE):
        return collective(nf, nt, *args)
    qd, vd, qm, vm, qc, vc, *new = exchange(nf, nr, nt, *args)
    return qd, vd, qm, vm, *new, qc, vc

def square(nf, nr, nt):
    return (nf, nr, nt) == (4, 2 * 2, 2)

def solution(mesh):
    placed = (
        P(("fs", "rep"), None),
        P(("fs", "rep"), "tp"),
        P(("fs", "rep"), "tp"),
        P("fs", "tp"),
        P("fs", "tp"),
        P("fs", None),
        P("fs", None),
        P("rep", "tp"),
        P("rep", "tp"),
        P("rep", "tp"),
        P("rep", "tp"),
    )
    return jax.shard_map(
        functools.partial(local, mesh.shape["fs"], mesh.shape["rep"], mesh.shape["tp"]),
        mesh=mesh,
        in_specs=placed,
        out_specs=(P("fs", "tp"),) * 4 + (P("rep", "tp"),) * 4 + (P(None, "tp"),) * 2,
        check_vma=False,
    )
```
